32 devices in a mesh: sp: 4 (over z), tp: 8 (over y, x, core).
Axes of the slice: x: 2, y: 2, z: 4, core: 2. Of those that a mesh axis runs over, the one named last changes fastest.
Arguments:
- activations: bfloat16 [1024, 2048], P('sp', 'tp'), may hold values from -170 to 170
- norm_gain: float32 [2048], replicated, may hold values from 0.1 to 1.9
- query_weight: bfloat16 [2048, 1536], P(None, 'tp'), may hold values from -0.125 to 0.125
- latent_weight: bfloat16 [2048, 512], P(None, 'tp'), may hold values from -0.125 to 0.125
- rope_key_weight: bfloat16 [2048, 64], replicated, may hold values from -0.125 to 0.125
- latent_gain: float32 [512], replicated, may hold values from 1.5 to 64
- expand_weight: bfloat16 [512, 2048], P(None, 'tp'), may hold values from -0.25 to 0.25
- gate_weight: bfloat16 [2048, 1024], P(None, 'tp'), may hold values from -0.125 to 0.125
- pre_weight: bfloat16 [2048, 1024], P(None, 'tp'), may hold values from -0.125 to 0.125
- value_weight: bfloat16 [2048, 1024], P(None, 'tp'), may hold values from -0.125 to 0.125
- conv_kernel: bfloat16 [3, 1024], P(None, 'tp'), may hold values from -3.5 to 3.5
- output_attend: bfloat16 [1024, 2048], P('tp'), may hold values from -0.1875 to 0.1875
- output_conv: bfloat16 [1024, 2048], P('tp'), may hold values from -0.125 to 0.125
Outputs:
- mixed: bfloat16 [1024, 2048], P(('sp', 'tp'))
- log_weight_sum: float32 [8, 1024], P('tp', 'sp')
The draws below stay inside these ranges and needn't reach their ends.
All inputs are finite; a program needn't handle non-finite values.
Results may differ from the reference program's by a relative error of at most 0.035.
The reference program's roundings to bfloat16 on the way count: a program that leaves them out, or rounds other values in their place, can miss the bound.
Values may be sent and summed in bfloat16 or wider, within the bound.
A program may use at most 128 MiB of HBM per device.

```python
import math
import jax
import jax.numpy as jnp
from jax import lax

D = 2048
HEADS = 8
NOPE = 128
ROPE = 64
VDIM = 128
KV_RANK = 512
CONV_CH = 1024
KERNEL = 3
GRID_W = 64
TOKENS = 1024
N_TP = 8


def draw_activations(key, part):
    noise_key = jax.random.fold_in(key, 11)
    scale_key = jax.random.fold_in(key, 12)
    steps_along = jnp.arange(D, dtype=jnp.float32) / D
    noise = jnp.clip(jax.random.normal(noise_key, (TOKENS, D), jnp.float32), -5.0, 5.0)
    column_scale = 3.0 ** steps_along
    row_scale = jnp.exp(jax.random.uniform(scale_key, (TOKENS, 1), jnp.float32, 0.0, 1.1))
    return (noise * column_scale * row_scale).astype(jnp.bfloat16)


def draw_latent_gain(key, part):
    gain_key = jax.random.fold_in(key, 21)
    lower_end = math.log(1.5)
    upper_end = math.log(6.0)
    return jnp.exp(jax.random.uniform(gain_key, (KV_RANK,), jnp.float32, lower_end, upper_end))


def level_of(rng, extent, cuts, least, largest):
    loudness, own = 1.0, jax.random.fold_in(rng, 6)
    for position, parts in cuts:
        heights = jnp.exp(jax.random.uniform(jax.random.fold_in(own, position), (parts,), jnp.float32, least / len(cuts), largest / len(cuts)))
        loudness = loudness * jnp.repeat(heights, extent[position] // parts).reshape([-1 if axis == position else 1 for axis in range(len(extent))])
    return loudness


def scatter_about(stream_key, shape, deviation, limit, shards=(), kind=jnp.bfloat16):
    entries = deviation * jax.random.normal(stream_key, shape, jnp.float32)
    if shards:
        entries = entries * level_of(stream_key, shape, shards, -0.22, 0.18)
    return jnp.clip(entries, -limit, limit).astype(kind)


def setup_inputs(seed: int = 0) -> dict:
    key_of = jax.random.split(jax.random.key(seed), 14)
    activations = draw_activations(jax.random.fold_in(key_of[13], 71), 0)
    norm_gain = jnp.clip(1.0 + 0.18 * jax.random.normal(key_of[1], (D,), jnp.float32), 0.1, 1.9)
    query_weight = scatter_about(key_of[2], (D, HEADS * (NOPE + ROPE)), D ** -0.5, 0.125, ((1, 8),))
    latent_weight = scatter_about(key_of[3], (D, KV_RANK), D ** -0.5, 0.125, ((1, 8),))
    rope_key_weight = scatter_about(key_of[4], (D, ROPE), D ** -0.5, 0.125)
    latent_gain = draw_latent_gain(jax.random.fold_in(key_of[13], 71), 0)
    expand_weight = scatter_about(key_of[6], (KV_RANK, HEADS * (NOPE + VDIM)), KV_RANK ** -0.5, 0.25, ((1, 8),))
    gate_weight = scatter_about(key_of[7], (D, CONV_CH), D ** -0.5, 0.125, ((1, 8),))
    pre_weight = scatter_about(key_of[8], (D, CONV_CH), D ** -0.5, 0.125, ((1, 8),))
    value_weight = scatter_about(key_of[9], (D, CONV_CH), D ** -0.5, 0.125, ((1, 8),))
    conv_kernel = scatter_about(key_of[10], (KERNEL, CONV_CH), KERNEL ** -0.5, 3.5, ((1, 8),))
    output_attend = scatter_about(key_of[11], (HEADS * VDIM, D), (HEADS * VDIM) ** -0.5, 0.1875, ((0, 8),))
    output_conv = scatter_about(key_of[12], (CONV_CH, D), (2 * CONV_CH) ** -0.5, 0.125, ((0, 8),))
    return {"activations": activations, "norm_gain": norm_gain, "query_weight": query_weight, "latent_weight": latent_weight, "rope_key_weight": rope_key_weight, "latent_gain": latent_gain, "expand_weight": expand_weight, "gate_weight": gate_weight, "pre_weight": pre_weight, "value_weight": value_weight, "conv_kernel": conv_kernel, "output_attend": output_attend, "output_conv": output_conv}


EPSILON = 1e-06
ROPE_BASE = 10000.0

def rotate(inputs, grid_rows, grid_cols):
    quarter = inputs.shape[-1] // 4
    inverse = ROPE_BASE ** (-jnp.arange(quarter, dtype=jnp.float32) / quarter)
    row_angle = (grid_rows[:, None] * inverse)[:, None, :]
    col_angle = (grid_cols[:, None] * inverse)[:, None, :]
    part_one = inputs[..., :quarter]
    part_two = inputs[..., quarter:2 * quarter]
    part_three = inputs[..., 2 * quarter:3 * quarter]
    part_four = inputs[..., 3 * quarter:]
    return jnp.concatenate([part_one * jnp.cos(row_angle) - part_two * jnp.sin(row_angle), part_one * jnp.sin(row_angle) + part_two * jnp.cos(row_angle), part_three * jnp.cos(col_angle) - part_four * jnp.sin(col_angle), part_three * jnp.sin(col_angle) + part_four * jnp.cos(col_angle)], axis=-1)

def reference(activations, norm_gain, query_weight, latent_weight, rope_key_weight, latent_gain, expand_weight, gate_weight, pre_weight, value_weight, conv_kernel, output_attend, output_conv):
    inputs_f32 = activations.astype(jnp.float32)
    scaled = (inputs_f32 * norm_gain).astype(jnp.bfloat16)
    inv_rms = lax.rsqrt(lax.optimization_barrier(jnp.mean(inputs_f32 * inputs_f32, axis=1, keepdims=True)) + EPSILON)

    def project(weight):
        return jnp.dot(scaled, weight, preferred_element_type=jnp.float32) * inv_rms
    positions = jnp.arange(TOKENS, dtype=jnp.int32)
    grid_rows = (positions // GRID_W).astype(jnp.float32)
    grid_cols = (positions % GRID_W).astype(jnp.float32)
    query = project(query_weight).reshape(TOKENS, HEADS, NOPE + ROPE)
    query = jnp.concatenate([query[..., :NOPE], rotate(query[..., NOPE:], grid_rows, grid_cols)], axis=-1)
    query = (query * (NOPE + ROPE) ** (-0.5)).astype(jnp.bfloat16)
    latent_part = project(latent_weight).astype(jnp.bfloat16).astype(jnp.float32)
    latent = (latent_part * lax.rsqrt(lax.optimization_barrier(jnp.mean(latent_part * latent_part, axis=1, keepdims=True)) + EPSILON) * latent_gain).astype(jnp.bfloat16)
    expanded = jnp.dot(latent, expand_weight, preferred_element_type=jnp.float32).astype(jnp.bfloat16)
    expanded = expanded.reshape(TOKENS, HEADS, NOPE + VDIM)
    rope_key = rotate(project(rope_key_weight)[:, None, :], grid_rows, grid_cols)[:, 0].astype(jnp.bfloat16)
    key_nope = expanded[..., :NOPE].astype(jnp.float32)
    values = expanded[..., NOPE:].astype(jnp.float32)
    rope_f32 = rope_key.astype(jnp.float32)
    query_block = math.gcd(TOKENS, 512)
    query_blocks = query.reshape(TOKENS // query_block, query_block, HEADS, NOPE + ROPE)

    def attend(block):
        block_f32 = block.astype(jnp.float32)
        scores = jnp.einsum('thd,jhd->htj', block_f32[..., :NOPE], key_nope)
        scores = scores + jnp.einsum('thd,jd->htj', block_f32[..., NOPE:], rope_f32)
        row_max = lax.optimization_barrier(jnp.max(scores, axis=-1))
        shifted = jnp.exp(scores - row_max[..., None])
        row_sum = lax.optimization_barrier(jnp.sum(shifted, axis=-1))
        weights = lax.optimization_barrier(shifted.astype(jnp.bfloat16)).astype(jnp.float32)
        summed = jnp.einsum('htj,jhd->thd', weights, values)
        attended_block = (summed / row_sum.T[..., None]).astype(jnp.bfloat16)
        return (attended_block, row_max + jnp.log(row_sum))
    attended_blocks, log_blocks = lax.map(attend, query_blocks)
    attended = attended_blocks.reshape(TOKENS, HEADS * VDIM)
    log_weight_sum = jnp.transpose(log_blocks, (1, 0, 2)).reshape(HEADS, TOKENS)
    pre_mix = (project(pre_weight) * project(value_weight)).astype(jnp.bfloat16).astype(jnp.float32)
    padded = jnp.pad(pre_mix, ((1, 1), (0, 0)))
    kernel = conv_kernel.astype(jnp.float32)
    convolved = kernel[0] * padded[:-2] + kernel[1] * padded[1:-1] + kernel[2] * padded[2:]
    conv_mixed = (project(gate_weight) * convolved).astype(jnp.bfloat16)
    attend_cols = HEADS * VDIM // N_TP
    conv_cols = CONV_CH // N_TP
    summed_out = jnp.zeros((TOKENS, D), jnp.float32)
    for group_index in range(N_TP):
        head_part = attended[:, group_index * attend_cols:(group_index + 1) * attend_cols]
        chan_part = conv_mixed[:, group_index * conv_cols:(group_index + 1) * conv_cols]
        partial_value = jnp.dot(head_part, output_attend[group_index * attend_cols:(group_index + 1) * attend_cols], preferred_element_type=jnp.float32)
        partial_value = partial_value + jnp.dot(chan_part, output_conv[group_index * conv_cols:(group_index + 1) * conv_cols], preferred_element_type=jnp.float32)
        summed_out = summed_out + lax.optimization_barrier(partial_value.astype(jnp.bfloat16)).astype(jnp.float32)
    mixed = summed_out.astype(jnp.bfloat16)
    return (mixed, log_weight_sum)
```

```python
import functools
import math

import jax
import jax.numpy as jnp
import numpy as np
from jax import lax
from jax.experimental import pallas as pl
from jax.experimental.pallas import tpu as pltpu
from jax.sharding import PartitionSpec as P

D = 2048
NOPE = 128
ROPE = 64
VDIM = 128
GRID_W = 64


EPSILON = 1e-06
ROPE_BASE = 10000.0


def with_halo(array, sides, width):
    for axis, dim in sides:
        peers, length = (lax.axis_size(axis), array.shape[dim])
        up = [(i, (i + 1) % peers) for i in range(peers - 1)]
        down = [(j, i) for i, j in up]
        last = lax.slice_in_dim(array, length - width, length, axis=dim)
        leading = lax.slice_in_dim(array, 0, width, axis=dim)
        before = lax.ppermute(last, axis, up)
        after = lax.ppermute(leading, axis, down)
        array = jnp.concatenate([before, array, after], axis=dim)
    return array


def rotate(inputs, grid_rows, grid_cols):
    quarter = inputs.shape[-1] // 4
    inverse = ROPE_BASE ** (-jnp.arange(quarter, dtype=jnp.float32) / quarter)
    row_angle = (grid_rows[:, None] * inverse)[:, None, :]
    col_angle = (grid_cols[:, None] * inverse)[:, None, :]
    part_one = inputs[..., :quarter]
    part_two = inputs[..., quarter : 2 * quarter]
    part_three = inputs[..., 2 * quarter : 3 * quarter]
    part_four = inputs[..., 3 * quarter :]
    return jnp.concatenate(
        [
            part_one * jnp.cos(row_angle) - part_two * jnp.sin(row_angle),
            part_one * jnp.sin(row_angle) + part_two * jnp.cos(row_angle),
            part_three * jnp.cos(col_angle) - part_four * jnp.sin(col_angle),
            part_three * jnp.sin(col_angle) + part_four * jnp.cos(col_angle),
        ],
        axis=-1,
    )


def conv_branch(gate_proj, pre_proj, value_proj, conv_kernel):
    pre_mix = (pre_proj * value_proj).astype(jnp.bfloat16)
    padded = with_halo(pre_mix, (("sp", 0),), 1).astype(jnp.float32)
    kernel = conv_kernel.astype(jnp.float32)
    convolved = kernel[0] * padded[:-2] + kernel[1] * padded[1:-1] + kernel[2] * padded[2:]
    return (gate_proj * convolved).astype(jnp.bfloat16)


def body(
    activations,
    norm_gain,
    query_weight,
    latent_weight,
    rope_key_weight,
    latent_gain,
    expand_weight,
    gate_weight,
    pre_weight,
    value_weight,
    conv_kernel,
    output_attend,
    output_conv,
):
    tokens_here = activations.shape[0]
    query_cols = query_weight.shape[1]
    heads_here = query_cols // (NOPE + ROPE)
    latent_cols = latent_weight.shape[1]
    channels = gate_weight.shape[1]
    joined = jnp.concatenate(
        [query_weight, latent_weight, rope_key_weight, gate_weight, pre_weight, value_weight],
        axis=1,
    )
    inputs_f32 = activations.astype(jnp.float32)
    squares = lax.psum(jnp.sum(inputs_f32 * inputs_f32, axis=1, keepdims=True), "tp")
    partial_squares = jnp.zeros((tokens_here, 1), jnp.float32)
    piece_f32 = lax.all_gather(activations, "tp", axis=1, tiled=True).astype(jnp.float32)
    scaled = (piece_f32 * norm_gain).astype(jnp.bfloat16)
    running = jnp.dot(scaled, joined, preferred_element_type=jnp.float32)
    running, folded_squares = (running, partial_squares)
    inv_rms = lax.rsqrt(squares / D + EPSILON)
    projected = running * inv_rms
    latent_end = query_cols + latent_cols
    rope_end = latent_end + ROPE
    query_proj = projected[:, :query_cols]
    latent_proj = projected[:, query_cols:latent_end]
    rope_proj = projected[:, latent_end:rope_end]
    gate_proj = projected[:, rope_end : rope_end + channels]
    pre_proj = projected[:, rope_end + channels : rope_end + 2 * channels]
    value_proj = projected[:, rope_end + 2 * channels :]
    positions = lax.axis_index("sp") * tokens_here + jnp.arange(tokens_here, dtype=jnp.int32)
    grid_rows = (positions // GRID_W).astype(jnp.float32)
    grid_cols = (positions % GRID_W).astype(jnp.float32)
    query = query_proj.reshape(tokens_here, heads_here, NOPE + ROPE)
    query = jnp.concatenate(
        [query[..., :NOPE], rotate(query[..., NOPE:], grid_rows, grid_cols)], axis=-1
    )
    query = (query * (NOPE + ROPE) ** (-0.5)).astype(jnp.bfloat16)
    query_nope = query[..., :NOPE]
    query_rope = query[..., NOPE:]
    gathered = lax.all_gather(latent_proj.astype(jnp.bfloat16), "tp", axis=1, tiled=True).astype(
        jnp.float32
    )
    latent = (
        gathered
        * lax.rsqrt(jnp.mean(gathered * gathered, axis=1, keepdims=True) + EPSILON)
        * latent_gain
    ).astype(jnp.bfloat16)
    expanded = jnp.dot(latent, expand_weight, preferred_element_type=jnp.float32).astype(
        jnp.bfloat16
    )
    rope_key = rotate(rope_proj[:, None, :], grid_rows, grid_cols)[:, 0].astype(jnp.bfloat16)
    starting = (
        jnp.full((heads_here, tokens_here), -jnp.inf, jnp.float32),
        jnp.zeros((heads_here, tokens_here), jnp.float32),
        jnp.zeros((tokens_here, heads_here, VDIM), jnp.float32),
    )
    key_piece = lax.all_gather(expanded, "sp", axis=0, tiled=True)
    rope_piece = lax.all_gather(rope_key, "sp", axis=0, tiled=True)
    piece_rows = key_piece.shape[0]
    key_block = math.gcd(piece_rows, 1024)
    split_heads = key_piece.reshape(piece_rows, heads_here, NOPE + VDIM)

    def one_block(turn_index, state):
        row_max, row_sum, running_out = state
        offset = turn_index * key_block
        block_keys = lax.dynamic_slice_in_dim(split_heads, offset, key_block, 0)
        block_rope = lax.dynamic_slice_in_dim(rope_piece, offset, key_block, 0)
        scores = jnp.einsum(
            "thd,jhd->htj", query_nope, block_keys[..., :NOPE], preferred_element_type=jnp.float32
        )
        scores = scores + jnp.einsum(
            "thd,jd->htj", query_rope, block_rope, preferred_element_type=jnp.float32
        )
        new_max = jnp.maximum(row_max, jnp.max(scores, axis=-1))
        rescale = jnp.exp(row_max - new_max)
        weights = jnp.exp(scores - new_max[..., None])
        row_sum = row_sum * rescale + jnp.sum(weights, axis=-1)
        running_out = running_out * rescale.T[..., None] + jnp.einsum(
            "htj,jhd->thd",
            weights.astype(jnp.bfloat16),
            block_keys[..., NOPE:],
            preferred_element_type=jnp.float32,
        )
        return (new_max, row_sum, running_out)

    row_max, row_sum, running_out = lax.fori_loop(0, piece_rows // key_block, one_block, starting)
    attended = (
        (running_out / row_sum.T[..., None])
        .astype(jnp.bfloat16)
        .reshape(tokens_here, heads_here * VDIM)
    )
    log_weight_sum = row_max + jnp.log(row_sum)
    conv_mixed = conv_branch(gate_proj, pre_proj, value_proj, conv_kernel)
    mixed = lax.psum_scatter(
        (
            jnp.dot(attended, output_attend, preferred_element_type=jnp.float32)
            + jnp.dot(conv_mixed, output_conv, preferred_element_type=jnp.float32)
        ).astype(jnp.bfloat16),
        "tp",
        scatter_dimension=0,
        tiled=True,
    )
    return (mixed, log_weight_sum)


CORES = 2
MAX_SPLITS = 8
OUT_CHUNKS = 4
MESH = pl.DeviceIdType.MESH


def fits(mesh):
    chips = mesh.shape["tp"] // CORES
    return mesh.shape["sp"] <= MAX_SPLITS and chips & (chips - 1) == 0


def flip(index, mask, count):
    total, bit = 0, 1
    while bit < count:
        has = (index // bit) % 2
        total = total + bit * ((1 - has) if mask & bit else has)
        bit *= 2
    return total


def rope_table(tokens):
    quarter = ROPE // 4
    inverse = np.float32(ROPE_BASE) ** (-np.arange(quarter, dtype=np.float32) / np.float32(quarter))
    place = np.arange(tokens)
    row = (place // GRID_W).astype(np.float32)[:, None] * inverse.astype(np.float32)
    col = (place % GRID_W).astype(np.float32)[:, None] * inverse.astype(np.float32)
    parts = [np.cos(row), np.cos(row), np.cos(col), np.cos(col)]
    parts += [-np.sin(row), np.sin(row), -np.sin(col), np.sin(col)]
    return np.concatenate(parts, axis=1).astype(np.float32)


def turn(z, cos, sin):
    lane = lax.broadcasted_iota(jnp.int32, z.shape, 1)
    quarter = ROPE // 4
    other = jnp.where(lane % (2 * quarter) < quarter, pltpu.roll(z, 128 - quarter, 1), pltpu.roll(z, quarter, 1))
    return z * cos + other * sin


def mixer_kernel(
    splits,
    chips,
    act,
    gain,
    wq_h,
    wl_h,
    wr_h,
    lat_gain,
    we_h,
    wg_h,
    wp_h,
    wv_h,
    taps,
    oa_h,
    oc_h,
    tab_h,
    out_ref,
    lse_ref,
    actb,
    wq,
    wl,
    wr,
    we,
    wg,
    wp,
    wv,
    wo,
    tab,
    acc_l,
    acc_g,
    acc_q,
    latb,
    ropeb,
    halo_out,
    halo_in,
    qcat,
    kcat,
    vals,
    scores,
    pads,
    pbuf,
    pair_in,
    pair_sum,
    chip_in,
    in_sem,
    act_send,
    act_recv,
    lat_send,
    lat_recv,
    rope_send,
    rope_recv,
    halo_send,
    halo_recv,
    pair_send,
    pair_recv,
    chip_send,
    chip_recv,
):
    f32, bf16 = jnp.float32, jnp.bfloat16
    sp, tp = lax.axis_index("sp"), lax.axis_index("tp")
    core, chip = tp % CORES, tp // CORES
    tokens, local = act.shape
    half = tokens // 2
    partner = (sp, chip * CORES + 1 - core)
    chip_of = [flip(chip, m, chips) for m in range(chips)]
    mate = [(sp, chip_of[m] * CORES + core) for m in range(chips)]
    far = [((sp + d) % splits, tp) for d in range(splits)]
    near_first = list(range(1, chips))
    far_first = near_first[::-1]

    def remote(source, target, send, recv, device):
        return pltpu.make_async_remote_copy(
            src_ref=source, dst_ref=target, send_sem=send, recv_sem=recv,
            device_id=device, device_id_type=MESH,
        )

    loads = [
        (act, actb.at[0, core]), (wl_h, wl), (wr_h, wr), (wq_h, wq), (wg_h, wg), (wp_h, wp), (wv_h, wv),
        (tab_h.at[pl.ds(sp * tokens, tokens)], tab), (we_h, we),
        (oa_h, wo.at[pl.ds(0, oa_h.shape[0])]), (oc_h, wo.at[pl.ds(oa_h.shape[0], oc_h.shape[0])]),
    ]
    loads = [pltpu.make_async_copy(a, b, in_sem.at[i]) for i, (a, b) in enumerate(loads)]
    for load in loads:
        load.start()

    barrier = pltpu.get_barrier_semaphore()
    peers = [partner] + mate[1:] + far[1:]
    for peer in peers:
        pl.semaphore_signal(barrier, inc=1, device_id=peer, device_id_type=MESH)
    pl.semaphore_wait(barrier, len(peers))

    pending = []
    loads[0].wait()
    own = actb.at[0, core]

    def send_act(m):
        copy = remote(own, actb.at[m, core], act_send.at[m], act_recv.at[m, 0], mate[m])
        copy.start()
        pending.append(copy)
        return copy

    def pass_act(m):
        copy = remote(actb.at[m, core], actb.at[m, core], act_send.at[chips + m], act_recv.at[m, 1], partner)
        copy.start()
        pending.append(copy)
        return copy

    direct = {m: send_act(m) for m in far_first}
    passed = {0: pass_act(0)}
    for load in loads[1:8]:
        load.wait()

    squares = jnp.zeros((tokens, 128), f32)
    scaled = {}

    def rows_of(m, k):
        return pl.ds(pl.multiple_of((chip_of[m] * CORES + k) * local, local), local)

    def scale(m, squares):
        for k in range(CORES):
            x = actb[m, k].astype(f32)
            for c in range(0, local, 128):
                squares = squares + x[:, c : c + 128] * x[:, c : c + 128]
            scaled[m, k] = (x * gain[:, rows_of(m, k)]).astype(bf16)
        return squares

    def put(ref, value, first):
        if first:
            ref[...] = value
        else:
            ref[...] += value

    def latent_dot(m):
        for k in range(CORES):
            rows = rows_of(m, k)
            weight = jnp.concatenate([wl[rows, :], wr[rows, :]], axis=1)
            put(acc_l, jnp.dot(scaled[m, k], weight, preferred_element_type=f32), m == 0 and k == 0)

    def other_dots(m):
        for k in range(CORES):
            rows = rows_of(m, k)
            first = m == 0 and k == 0
            weight = jnp.concatenate([wg[rows, :], wp[rows, :], wv[rows, :]], axis=1)
            put(acc_g, jnp.dot(scaled[m, k], weight, preferred_element_type=f32), first)
            put(acc_q, jnp.dot(scaled[m, k], wq[rows, :], preferred_element_type=f32), first)

    passed[0].wait_recv()
    squares = scale(0, squares)
    latent_dot(0)
    other_dots(0)
    for m in near_first:
        direct[m].wait_recv()
        passed[m] = pass_act(m)
        if m > 1:
            passed[m - 1].wait_recv()
            squares = scale(m - 1, squares)
            latent_dot(m - 1)
            other_dots(m - 1)
    last = chips - 1
    passed[last].wait_recv()
    squares = scale(last, squares)
    latent_dot(last)
    inv_rms = lax.rsqrt(jnp.sum(squares, axis=1, keepdims=True) / (local * chips * CORES) + EPSILON)

    lane = lax.broadcasted_iota(jnp.int32, (half, 128), 1)
    proj = acc_l[...] * inv_rms
    low, high = proj[:half], proj[half:]
    latb[0, 0, core] = jnp.where(lane < 64, low, pltpu.roll(high, 64, 1)).astype(bf16)

    def send_lat(d, m, index, recv, device, slot):
        copy = remote(latb.at[d, m, core], latb.at[slot[0], slot[1], core], lat_send.at[index], recv, device)
        copy.start()
        pending.append(copy)
        return copy

    count = 0
    lat_direct, lat_pass, lat_far = {}, {}, {}
    for d in [d for d in (2, 1, 3) if d < splits] + list(range(4, splits)):
        lat_far[d] = send_lat(0, 0, count, lat_recv.at[(splits - d) % splits, 0, 0], far[d], ((splits - d) % splits, 0))
        count += 1

    def spread(d, count):
        for m in far_first:
            lat_direct[d, m] = send_lat(d, 0, count, lat_recv.at[d, m, 0], mate[m], (d, m))
            count += 1
        lat_pass[d, 0] = send_lat(d, 0, count, lat_recv.at[d, 0, 1], partner, (d, 0))
        return count + 1

    count = spread(0, count)

    table = tab[...]
    wide = lax.broadcasted_iota(jnp.int32, (tokens, 128), 1)
    shifted = pltpu.roll(table, 64, 1)
    cos = jnp.where(wide < 64, table, shifted)
    sin = jnp.where(wide < 64, shifted, table)
    raw = jnp.where(lane < 64, pltpu.roll(low, 64, 1), high)
    ropeb[0] = turn(
        raw,
        jnp.where(lane < 64, cos[:half], cos[half:]),
        jnp.where(lane < 64, sin[:half], sin[half:]),
    ).astype(bf16)
    rope_far = {}
    for d in range(1, splits):
        back = (splits - d) % splits
        rope_far[back] = remote(ropeb.at[0], ropeb.at[back], rope_send.at[d], rope_recv.at[back], far[d])
        rope_far[back].start()
        pending.append(rope_far[back])

    other_dots(last)

    def far_wait(d):
        lat_far[(splits - d) % splits].wait_recv()

    premix = (acc_g[:, 128:256] * inv_rms) * (acc_g[:, 256:] * inv_rms)
    premix = premix.astype(bf16)
    rim = halo_out.shape[1]
    halo_out[0] = premix[tokens - rim :]
    halo_out[1] = premix[:rim]
    halos = [
        remote(halo_out.at[0], halo_in.at[0], halo_send.at[0], halo_recv.at[0], far[1]),
        remote(halo_out.at[1], halo_in.at[1], halo_send.at[1], halo_recv.at[1], far[splits - 1]),
    ]
    for copy in halos:
        copy.start()
        pending.append(copy)

    order = [0] + [d for d in (1, 3, 2) if d < splits] + list(range(4, splits))
    for d in order[1:]:
        far_wait(d)
        count = spread(d, count)

    factor = (NOPE + ROPE) ** (-0.5)
    qcat[:, :NOPE] = (acc_q[:, :NOPE] * inv_rms * factor).astype(bf16)
    tail = jnp.concatenate([acc_q[:, NOPE:], jnp.zeros((tokens, 128 - ROPE), f32)], axis=1) * inv_rms
    qcat[:, NOPE:] = jnp.where(wide < 64, turn(tail, cos, sin) * factor, 0.0).astype(bf16)

    for load in loads[8:]:
        load.wait()

    def pass_lat(d, count):
        for m in near_first:
            lat_direct[d, m].wait_recv()
            lat_pass[d, m] = send_lat(d, m, count, lat_recv.at[d, m, 1], partner, (d, m))
            count += 1
        return count

    def conv():
        pads[8 : 8 + tokens] = premix.astype(f32)
        for copy in halos:
            copy.wait_recv()
        before = jnp.where(sp > 0, halo_in[0].astype(f32)[rim - 1 :], 0.0)
        after = jnp.where(sp < splits - 1, halo_in[1].astype(f32)[:1], 0.0)
        pads[7:8] = before
        pads[8 + tokens : 9 + tokens] = after
        tap = taps[...].astype(f32)
        mixed = tap[0:1] * pads[7 : 7 + tokens] + tap[1:2] * pads[8 : 8 + tokens] + tap[2:3] * pads[9 : 9 + tokens]
        return ((acc_g[:, :128] * inv_rms) * mixed).astype(bf16)

    def expand(d):
        low, high = [], []
        weight = []
        for m in range(chips):
            a, b = latb[d, m, 0].astype(f32), latb[d, m, 1].astype(f32)
            low.append(jnp.where(lane < 64, a, pltpu.roll(b, 64, 1)))
            high.append(jnp.where(lane < 64, pltpu.roll(a, 64, 1), b))
            weight.append(we[pl.ds(pl.multiple_of(chip_of[m] * 128, 128), 128), :])
        weight = jnp.concatenate(weight, axis=0)
        for side, parts in enumerate((low, high)):
            total = sum(p * p for p in parts)
            root = lax.rsqrt(jnp.sum(total, axis=1, keepdims=True) / (128 * chips) + EPSILON)
            parts = [
                (p * root * lat_gain[:, pl.ds(pl.multiple_of(chip_of[m] * 128, 128), 128)]).astype(bf16)
                for m, p in enumerate(parts)
            ]
            result = jnp.dot(jnp.concatenate(parts, axis=1), weight, preferred_element_type=f32).astype(bf16)
            kcat[d, pl.ds(side * half, half), :NOPE] = result[:, :NOPE]
            vals[pl.ds(d * tokens + side * half, half), :] = result[:, NOPE:]

    def score(d):
        if d > 0:
            rope_far[d].wait_recv()
        packed = ropeb[d].astype(f32)
        kcat[d, pl.ds(0, half), NOPE:] = packed.astype(bf16)
        kcat[d, pl.ds(half, half), NOPE:] = pltpu.roll(packed, 64, 1).astype(bf16)
        scores[:, d * tokens : (d + 1) * tokens] = lax.dot_general(
            qcat[...], kcat[d], (((1,), (1,)), ((), ())), preferred_element_type=f32
        )

    conv_mixed = conv()
    previous = None
    for d in order:
        count = pass_lat(d, count)
        if previous is not None:
            for m in range(chips):
                lat_pass[previous, m].wait_recv()
            expand(previous)
            score(previous)
        previous = d
    for m in range(chips):
        lat_pass[previous, m].wait_recv()
    expand(previous)
    score(previous)

    s = scores[...]
    row_max = jnp.max(s, axis=1, keepdims=True)
    e = jnp.exp(s - row_max)
    row_sum = jnp.sum(e, axis=1, keepdims=True)
    summed = jnp.dot(e.astype(bf16), vals[...], preferred_element_type=f32)
    attended = (summed / row_sum).astype(bf16)
    both = jnp.concatenate([attended, conv_mixed], axis=1)

    slice_rows = tokens // (chips * CORES)
    width = wo.shape[1] // OUT_CHUNKS
    pairs, crosses = {}, {}
    for j in range(OUT_CHUNKS):
        cols = pl.ds(j * width, width)
        pbuf[:, cols] = jnp.dot(both, wo[:, cols], preferred_element_type=f32).astype(bf16)
        for m in far_first + [0]:
            rows = pl.ds(pl.multiple_of((chip_of[m] * CORES + 1 - core) * slice_rows, slice_rows), slice_rows)
            pairs[j, m] = remote(
                pbuf.at[rows, cols], pair_in.at[m, :, cols], pair_send.at[j, m], pair_recv.at[j, m], partner
            )
            pairs[j, m].start()
            pending.append(pairs[j, m])
    lse = row_max + jnp.log(row_sum)
    lse_ref[...] = jnp.transpose(jnp.broadcast_to(lse, (tokens, 128)))[:1]

    def mine(m, cols):
        rows = pl.ds(pl.multiple_of((chip_of[m] * CORES + core) * slice_rows, slice_rows), slice_rows)
        return pbuf[rows, cols].astype(f32) + pair_in[m, :, cols].astype(f32)

    for j in range(OUT_CHUNKS):
        cols = pl.ds(j * width, width)
        for m in far_first:
            pairs[j, m].wait_recv()
            pair_sum[m, :, cols] = mine(m, cols).astype(bf16)
            crosses[j, m] = remote(
                pair_sum.at[m, :, cols], chip_in.at[m, :, cols], chip_send.at[j, m], chip_recv.at[j, m], mate[m]
            )
            crosses[j, m].start()
            pending.append(crosses[j, m])
    for j in range(OUT_CHUNKS):
        cols = pl.ds(j * width, width)
        pairs[j, 0].wait_recv()
        total = mine(0, cols)
        for m in near_first:
            crosses[j, m].wait_recv()
            total = total + chip_in[m, :, cols].astype(f32)
        out_ref[:, cols] = total.astype(bf16)
    for copy in pending:
        copy.wait_send()


def fused(
    mesh,
    activations,
    norm_gain,
    query_weight,
    latent_weight,
    rope_key_weight,
    latent_gain,
    expand_weight,
    gate_weight,
    pre_weight,
    value_weight,
    conv_kernel,
    output_attend,
    output_conv,
):
    splits, chips = mesh.shape["sp"], mesh.shape["tp"] // CORES
    tokens, local = activations.shape
    width = output_attend.shape[1]
    bf16, f32 = jnp.bfloat16, jnp.float32
    slice_rows = tokens // (chips * CORES)
    table = jnp.asarray(rope_table(splits * tokens))
    vmem, hbm = pl.BlockSpec(memory_space=pltpu.VMEM), pl.BlockSpec(memory_space=pltpu.HBM)
    dma = pltpu.SemaphoreType.DMA
    whole = [query_weight, latent_weight, rope_key_weight, expand_weight, gate_weight, pre_weight, value_weight]
    return pl.pallas_call(
        functools.partial(mixer_kernel, splits, chips),
        out_shape=(
            jax.ShapeDtypeStruct((slice_rows, width), bf16),
            jax.ShapeDtypeStruct((1, tokens), f32),
        ),
        in_specs=[hbm, vmem, hbm, hbm, hbm, vmem, hbm, hbm, hbm, hbm, vmem, hbm, hbm, hbm],
        out_specs=(vmem, vmem),
        scratch_shapes=[pltpu.VMEM((chips, CORES, tokens, local), bf16)]
        + [pltpu.VMEM(w.shape, bf16) for w in whole]
        + [
            pltpu.VMEM((output_attend.shape[0] + output_conv.shape[0], width), bf16),
            pltpu.VMEM((tokens, 2 * ROPE), f32),
            pltpu.VMEM((tokens, 128), f32),
            pltpu.VMEM((tokens, 3 * 128), f32),
            pltpu.VMEM((tokens, NOPE + ROPE), f32),
            pltpu.VMEM((splits, chips, CORES, tokens // 2, 128), bf16),
            pltpu.VMEM((splits, tokens // 2, 128), bf16),
            pltpu.VMEM((2, 16, 128), bf16),
            pltpu.VMEM((2, 16, 128), bf16),
            pltpu.VMEM((tokens, 256), bf16),
            pltpu.VMEM((splits, tokens, 256), bf16),
            pltpu.VMEM((splits * tokens, VDIM), bf16),
            pltpu.VMEM((tokens, splits * tokens), f32),
            pltpu.VMEM((tokens + 16, 128), f32),
            pltpu.VMEM((tokens, width), bf16),
            pltpu.VMEM((chips, slice_rows, width), bf16),
            pltpu.VMEM((chips, slice_rows, width), bf16),
            pltpu.VMEM((chips, slice_rows, width), bf16),
            dma((11,)),
            dma((2 * chips,)),
            dma((chips, 2)),
            dma((splits * (2 * chips + 1),)),
            dma((splits, chips, 2)),
            dma((splits,)),
            dma((splits,)),
            dma((2,)),
            dma((2,)),
            dma((OUT_CHUNKS, chips)),
            dma((OUT_CHUNKS, chips)),
            dma((OUT_CHUNKS, chips)),
            dma((OUT_CHUNKS, chips)),
        ],
        compiler_params=pltpu.CompilerParams(
            collective_id=0, has_side_effects=True, vmem_limit_bytes=60 * 2**20
        ),
    )(
        activations,
        norm_gain[None],
        query_weight,
        latent_weight,
        rope_key_weight,
        latent_gain[None],
        expand_weight,
        gate_weight,
        pre_weight,
        value_weight,
        conv_kernel,
        output_attend,
        output_conv,
        table,
    )


def solution(mesh):
    return jax.shard_map(
        functools.partial(fused, mesh) if fits(mesh) else body,
        mesh=mesh,
        in_specs=(
            P("sp", "tp"),
            P(),
            P(None, "tp"),
            P(None, "tp"),
            P(),
            P(),
            P(None, "tp"),
            P(None, "tp"),
            P(None, "tp"),
            P(None, "tp"),
            P(None, "tp"),
            P("tp", None),
            P("tp", None),
        ),
        out_specs=(P(("sp", "tp"), None), P("tp", "sp")),
        check_vma=False,
    )
```

```python
import functools
import math

import jax
import jax.numpy as jnp
import numpy as np
from jax import lax
from jax.experimental import pallas as pl
from jax.experimental.pallas import tpu as pltpu
from jax.sharding import PartitionSpec as P

D = 2048
NOPE = 128
ROPE = 64
VDIM = 128
GRID_W = 64


EPSILON = 1e-06
ROPE_BASE = 10000.0


def with_halo(array, sides, width):
    for axis, dim in sides:
        peers, length = (lax.axis_size(axis), array.shape[dim])
        up = [(i, (i + 1) % peers) for i in range(peers - 1)]
        down = [(j, i) for i, j in up]
        last = lax.slice_in_dim(array, length - width, length, axis=dim)
        leading = lax.slice_in_dim(array, 0, width, axis=dim)
        before = lax.ppermute(last, axis, up)
        after = lax.ppermute(leading, axis, down)
        array = jnp.concatenate([before, array, after], axis=dim)
    return array


def rotate(inputs, grid_rows, grid_cols):
    quarter = inputs.shape[-1] // 4
    inverse = ROPE_BASE ** (-jnp.arange(quarter, dtype=jnp.float32) / quarter)
    row_angle = (grid_rows[:, None] * inverse)[:, None, :]
    col_angle = (grid_cols[:, None] * inverse)[:, None, :]
    part_one = inputs[..., :quarter]
    part_two = inputs[..., quarter : 2 * quarter]
    part_three = inputs[..., 2 * quarter : 3 * quarter]
    part_four = inputs[..., 3 * quarter :]
    return jnp.concatenate(
        [
            part_one * jnp.cos(row_angle) - part_two * jnp.sin(row_angle),
            part_one * jnp.sin(row_angle) + part_two * jnp.cos(row_angle),
            part_three * jnp.cos(col_angle) - part_four * jnp.sin(col_angle),
            part_three * jnp.sin(col_angle) + part_four * jnp.cos(col_angle),
        ],
        axis=-1,
    )


def conv_branch(gate_proj, pre_proj, value_proj, conv_kernel):
    pre_mix = (pre_proj * value_proj).astype(jnp.bfloat16)
    padded = with_halo(pre_mix, (("sp", 0),), 1).astype(jnp.float32)
    kernel = conv_kernel.astype(jnp.float32)
    convolved = kernel[0] * padded[:-2] + kernel[1] * padded[1:-1] + kernel[2] * padded[2:]
    return (gate_proj * convolved).astype(jnp.bfloat16)


def body(
    activations,
    norm_gain,
    query_weight,
    latent_weight,
    rope_key_weight,
    latent_gain,
    expand_weight,
    gate_weight,
    pre_weight,
    value_weight,
    conv_kernel,
    output_attend,
    output_conv,
):
    tokens_here = activations.shape[0]
    query_cols = query_weight.shape[1]
    heads_here = query_cols // (NOPE + ROPE)
    latent_cols = latent_weight.shape[1]
    channels = gate_weight.shape[1]
    joined = jnp.concatenate(
        [query_weight, latent_weight, rope_key_weight, gate_weight, pre_weight, value_weight],
        axis=1,
    )
    inputs_f32 = activations.astype(jnp.float32)
    squares = lax.psum(jnp.sum(inputs_f32 * inputs_f32, axis=1, keepdims=True), "tp")
    partial_squares = jnp.zeros((tokens_here, 1), jnp.float32)
    piece_f32 = lax.all_gather(activations, "tp", axis=1, tiled=True).astype(jnp.float32)
    scaled = (piece_f32 * norm_gain).astype(jnp.bfloat16)
    running = jnp.dot(scaled, joined, preferred_element_type=jnp.float32)
    running, folded_squares = (running, partial_squares)
    inv_rms = lax.rsqrt(squares / D + EPSILON)
    projected = running * inv_rms
    latent_end = query_cols + latent_cols
    rope_end = latent_end + ROPE
    query_proj = projected[:, :query_cols]
    latent_proj = projected[:, query_cols:latent_end]
    rope_proj = projected[:, latent_end:rope_end]
    gate_proj = projected[:, rope_end : rope_end + channels]
    pre_proj = projected[:, rope_end + channels : rope_end + 2 * channels]
    value_proj = projected[:, rope_end + 2 * channels :]
    positions = lax.axis_index("sp") * tokens_here + jnp.arange(tokens_here, dtype=jnp.int32)
    grid_rows = (positions // GRID_W).astype(jnp.float32)
    grid_cols = (positions % GRID_W).astype(jnp.float32)
    query = query_proj.reshape(tokens_here, heads_here, NOPE + ROPE)
    query = jnp.concatenate(
        [query[..., :NOPE], rotate(query[..., NOPE:], grid_rows, grid_cols)], axis=-1
    )
    query = (query * (NOPE + ROPE) ** (-0.5)).astype(jnp.bfloat16)
    query_nope = query[..., :NOPE]
    query_rope = query[..., NOPE:]
    gathered = lax.all_gather(latent_proj.astype(jnp.bfloat16), "tp", axis=1, tiled=True).astype(
        jnp.float32
    )
    latent = (
        gathered
        * lax.rsqrt(jnp.mean(gathered * gathered, axis=1, keepdims=True) + EPSILON)
        * latent_gain
    ).astype(jnp.bfloat16)
    expanded = jnp.dot(latent, expand_weight, preferred_element_type=jnp.float32).astype(
        jnp.bfloat16
    )
    rope_key = rotate(rope_proj[:, None, :], grid_rows, grid_cols)[:, 0].astype(jnp.bfloat16)
    starting = (
        jnp.full((heads_here, tokens_here), -jnp.inf, jnp.float32),
        jnp.zeros((heads_here, tokens_here), jnp.float32),
        jnp.zeros((tokens_here, heads_here, VDIM), jnp.float32),
    )
    key_piece = lax.all_gather(expanded, "sp", axis=0, tiled=True)
    rope_piece = lax.all_gather(rope_key, "sp", axis=0, tiled=True)
    piece_rows = key_piece.shape[0]
    key_block = math.gcd(piece_rows, 1024)
    split_heads = key_piece.reshape(piece_rows, heads_here, NOPE + VDIM)

    def one_block(turn_index, state):
        row_max, row_sum, running_out = state
        offset = turn_index * key_block
        block_keys = lax.dynamic_slice_in_dim(split_heads, offset, key_block, 0)
        block_rope = lax.dynamic_slice_in_dim(rope_piece, offset, key_block, 0)
        scores = jnp.einsum(
            "thd,jhd->htj", query_nope, block_keys[..., :NOPE], preferred_element_type=jnp.float32
        )
        scores = scores + jnp.einsum(
            "thd,jd->htj", query_rope, block_rope, preferred_element_type=jnp.float32
        )
        new_max = jnp.maximum(row_max, jnp.max(scores, axis=-1))
        rescale = jnp.exp(row_max - new_max)
        weights = jnp.exp(scores - new_max[..., None])
        row_sum = row_sum * rescale + jnp.sum(weights, axis=-1)
        running_out = running_out * rescale.T[..., None] + jnp.einsum(
            "htj,jhd->thd",
            weights.astype(jnp.bfloat16),
            block_keys[..., NOPE:],
            preferred_element_type=jnp.float32,
        )
        return (new_max, row_sum, running_out)

    row_max, row_sum, running_out = lax.fori_loop(0, piece_rows // key_block, one_block, starting)
    attended = (
        (running_out / row_sum.T[..., None])
        .astype(jnp.bfloat16)
        .reshape(tokens_here, heads_here * VDIM)
    )
    log_weight_sum = row_max + jnp.log(row_sum)
    conv_mixed = conv_branch(gate_proj, pre_proj, value_proj, conv_kernel)
    mixed = lax.psum_scatter(
        (
            jnp.dot(attended, output_attend, preferred_element_type=jnp.float32)
            + jnp.dot(conv_mixed, output_conv, preferred_element_type=jnp.float32)
        ).astype(jnp.bfloat16),
        "tp",
        scatter_dimension=0,
        tiled=True,
    )
    return (mixed, log_weight_sum)


CORES = 2
VMEM_LIMIT = 60 * 2**20
MAX_SPLITS = 8
OUT_CHUNKS = 4
MESH = pl.DeviceIdType.MESH


def fits(mesh):
    chips = mesh.shape["tp"] // CORES
    return mesh.shape["sp"] <= MAX_SPLITS and chips == 4


def flip(index, mask, count):
    total, bit = 0, 1
    while bit < count:
        has = (index // bit) % 2
        total = total + bit * ((1 - has) if mask & bit else has)
        bit *= 2
    return total


def rope_table(tokens):
    quarter = ROPE // 4
    inverse = np.float32(ROPE_BASE) ** (-np.arange(quarter, dtype=np.float32) / np.float32(quarter))
    place = np.arange(tokens)
    row = (place // GRID_W).astype(np.float32)[:, None] * inverse.astype(np.float32)
    col = (place % GRID_W).astype(np.float32)[:, None] * inverse.astype(np.float32)
    parts = [np.cos(row), np.cos(row), np.cos(col), np.cos(col)]
    parts += [-np.sin(row), np.sin(row), -np.sin(col), np.sin(col)]
    return np.concatenate(parts, axis=1).astype(np.float32)


def turn(z, cos, sin):
    lane = lax.broadcasted_iota(jnp.int32, z.shape, 1)
    quarter = ROPE // 4
    other = jnp.where(lane % (2 * quarter) < quarter, pltpu.roll(z, 128 - quarter, 1), pltpu.roll(z, quarter, 1))
    return z * cos + other * sin


def mixer_kernel(
    splits,
    chips,
    act,
    gain,
    wq_h,
    wl_h,
    wr_h,
    lat_gain,
    we_h,
    wg_h,
    wp_h,
    wv_h,
    taps,
    oa_h,
    oc_h,
    tab_h,
    out_ref,
    lse_ref,
    actb,
    wq,
    wlr,
    we,
    wg,
    wp,
    wv,
    wo,
    tab,
    acc_l,
    acc_g,
    acc_q,
    latb,
    ropeb,
    halo_out,
    halo_in,
    qcat,
    kcat,
    vals,
    scores,
    pads,
    pbuf,
    pair_in,
    pair_sum,
    chip_in,
    in_sem,
    act_send,
    act_recv,
    lat_send,
    lat_recv,
    rope_send,
    rope_recv,
    halo_send,
    halo_recv,
    pair_send,
    pair_recv,
    chip_send,
    chip_recv,
):
    f32, bf16 = jnp.float32, jnp.bfloat16
    sp, tp = lax.axis_index("sp"), lax.axis_index("tp")
    core, chip = tp % CORES, tp // CORES
    tokens, local = act.shape
    half = tokens // 2
    partner = (sp, chip * CORES + 1 - core)
    chip_of = [flip(chip, m, chips) for m in range(chips)]
    mate = [(sp, chip_of[m] * CORES + core) for m in range(chips)]
    far = [((sp + d) % splits, tp) for d in range(splits)]
    near_first = list(range(1, chips))
    far_first = near_first[::-1]

    def remote(source, target, send, recv, device):
        return pltpu.make_async_remote_copy(
            src_ref=source, dst_ref=target, send_sem=send, recv_sem=recv,
            device_id=device, device_id_type=MESH,
        )

    loads = [
        (act, actb.at[0, core]), (wl_h, wlr.at[pl.ds(0, wl_h.shape[0])]), (wr_h, wlr.at[pl.ds(wl_h.shape[0], wr_h.shape[0])]), (wq_h, wq), (wg_h, wg), (wp_h, wp), (wv_h, wv),
        (tab_h.at[pl.ds(sp * tokens, tokens)], tab), (we_h, we),
        (oa_h, wo.at[pl.ds(0, oa_h.shape[0])]), (oc_h, wo.at[pl.ds(oa_h.shape[0], oc_h.shape[0])]),
    ]
    loads = [pltpu.make_async_copy(a, b, in_sem.at[i]) for i, (a, b) in enumerate(loads)]
    for load in loads:
        load.start()

    barrier = pltpu.get_barrier_semaphore()
    peers = [partner] + mate[1:] + far[1:]
    for peer in peers:
        pl.semaphore_signal(barrier, inc=1, device_id=peer, device_id_type=MESH)
    pl.semaphore_wait(barrier, len(peers))

    pending = []
    loads[0].wait()
    own = actb.at[0, core]

    def act_copy(m, slot, side, kind, device, index):
        piece = pl.ds(side * half, half)
        copy = remote(
            actb.at[m, core, piece], actb.at[slot, core, piece], act_send.at[index], act_recv.at[slot, side, kind], device
        )
        copy.start()
        pending.append(copy)
        return copy

    direct, passed = {}, {}
    for index, (m, side) in enumerate([(1, 0), (2, 1), (1, 1), (2, 0)]):
        direct[m, side] = act_copy(0, m, side, 0, mate[m], index)
    for side in range(2):
        passed[0, side] = act_copy(0, 0, side, 1, partner, 4 + side)
    for load in loads[1:8]:
        load.wait()

    squares = jnp.zeros((tokens, 128), f32)
    scaled = {}

    def rows_of(m, k):
        return pl.ds(pl.multiple_of((chip_of[m] * CORES + k) * local, local), local)

    def scale(m, squares):
        for k in range(CORES):
            x = actb[m, k].astype(f32)
            for c in range(0, local, 128):
                squares = squares + x[:, c : c + 128] * x[:, c : c + 128]
            scaled[m, k] = (x * gain[:, rows_of(m, k)]).astype(bf16)
        return squares

    def put(ref, value, first):
        if first:
            ref[...] = value
        else:
            ref[...] += value

    def across(left, right):
        return lax.dot_general(left, right, (((1,), (1,)), ((), ())), preferred_element_type=f32)

    def latent_dot(m):
        for k in range(CORES):
            rows = rows_of(m, k)
            put(acc_l, across(scaled[m, k], wlr[:, rows]), m == 0 and k == 0)

    def other_dots(m):
        for k in range(CORES):
            rows = rows_of(m, k)
            first = m == 0 and k == 0
            weight = jnp.concatenate([wg[rows, :], wp[rows, :], wv[rows, :]], axis=1)
            put(acc_g, jnp.dot(scaled[m, k], weight, preferred_element_type=f32), first)
            put(acc_q, across(scaled[m, k], wq[:, rows]), first)

    def arrived(m):
        for side in range(2):
            passed[m, side].wait_recv()

    def take(m, squares, others=True):
        arrived(m)
        squares = scale(m, squares)
        latent_dot(m)
        if others:
            other_dots(m)
        return squares

    squares = take(0, squares)
    for index, (m, side) in enumerate([(1, 0), (2, 1), (1, 1), (2, 0)]):
        direct[m, side].wait_recv()
        if index < 2:
            direct[3, side] = act_copy(m, 3, side, 0, mate[3 - m], 6 + index)
        passed[m, side] = act_copy(m, m, side, 1, partner, 8 + index)
    squares = take(1, squares)
    for side in range(2):
        direct[3, side].wait_recv()
        passed[3, side] = act_copy(3, 3, side, 1, partner, 12 + side)
    squares = take(2, squares)
    last = chips - 1
    squares = take(last, squares, False)
    inv_rms = lax.rsqrt(jnp.sum(squares, axis=1, keepdims=True) / (local * chips * CORES) + EPSILON)

    lane = lax.broadcasted_iota(jnp.int32, (half, 128), 1)
    proj = acc_l[...] * inv_rms
    low, high = proj[:half], proj[half:]
    latb[0, 0, core] = jnp.where(lane < 64, low, pltpu.roll(high, 64, 1)).astype(bf16)

    def send_lat(d, m, index, recv, device, slot):
        copy = remote(latb.at[d, m, core], latb.at[slot[0], slot[1], core], lat_send.at[index], recv, device)
        copy.start()
        pending.append(copy)
        return copy

    count = 0
    lat_direct, lat_pass, lat_far = {}, {}, {}
    for d in [d for d in (2, 1, 3) if d < splits] + list(range(4, splits)):
        lat_far[d] = send_lat(0, 0, count, lat_recv.at[(splits - d) % splits, 0, 0], far[d], ((splits - d) % splits, 0))
        count += 1

    def spread(d, count):
        for m in far_first:
            lat_direct[d, m] = send_lat(d, 0, count, lat_recv.at[d, m, 0], mate[m], (d, m))
            count += 1
        lat_pass[d, 0] = send_lat(d, 0, count, lat_recv.at[d, 0, 1], partner, (d, 0))
        return count + 1

    count = spread(0, count)

    table = tab[...]
    wide = lax.broadcasted_iota(jnp.int32, (tokens, 128), 1)
    shifted = pltpu.roll(table, 64, 1)
    cos = jnp.where(wide < 64, table, shifted)
    sin = jnp.where(wide < 64, shifted, table)
    raw = jnp.where(lane < 64, pltpu.roll(low, 64, 1), high)
    ropeb[0] = turn(
        raw,
        jnp.where(lane < 64, cos[:half], cos[half:]),
        jnp.where(lane < 64, sin[:half], sin[half:]),
    ).astype(bf16)
    rope_far = {}
    for d in range(1, splits):
        back = (splits - d) % splits
        rope_far[back] = remote(ropeb.at[0], ropeb.at[back], rope_send.at[d], rope_recv.at[back], far[d])
        rope_far[back].start()
        pending.append(rope_far[back])

    other_dots(last)

    def far_wait(d):
        lat_far[(splits - d) % splits].wait_recv()

    premix = (acc_g[:, 128:256] * inv_rms) * (acc_g[:, 256:] * inv_rms)
    premix = premix.astype(bf16)
    rim = halo_out.shape[1]
    halo_out[0] = premix[tokens - rim :]
    halo_out[1] = premix[:rim]
    halos = [
        remote(halo_out.at[0], halo_in.at[0], halo_send.at[0], halo_recv.at[0], far[1]),
        remote(halo_out.at[1], halo_in.at[1], halo_send.at[1], halo_recv.at[1], far[splits - 1]),
    ]
    for copy in halos:
        copy.start()
        pending.append(copy)

    order = [0] + [d for d in (1, 3, 2) if d < splits] + list(range(4, splits))
    for d in order[1:]:
        far_wait(d)
        count = spread(d, count)

    factor = (NOPE + ROPE) ** (-0.5)
    qcat[:, :NOPE] = (acc_q[:, :NOPE] * inv_rms * factor).astype(bf16)
    tail = jnp.concatenate([acc_q[:, NOPE:], jnp.zeros((tokens, 128 - ROPE), f32)], axis=1) * inv_rms
    qcat[:, NOPE:] = jnp.where(wide < 64, turn(tail, cos, sin) * factor, 0.0).astype(bf16)

    for load in loads[8:]:
        load.wait()

    def pass_lat(d, count):
        for m in near_first:
            lat_direct[d, m].wait_recv()
            lat_pass[d, m] = send_lat(d, m, count, lat_recv.at[d, m, 1], partner, (d, m))
            count += 1
        return count

    def conv():
        pads[8 : 8 + tokens] = premix.astype(f32)
        for copy in halos:
            copy.wait_recv()
        before = jnp.where(sp > 0, halo_in[0].astype(f32)[rim - 1 :], 0.0)
        after = jnp.where(sp < splits - 1, halo_in[1].astype(f32)[:1], 0.0)
        pads[7:8] = before
        pads[8 + tokens : 9 + tokens] = after
        tap = taps[...].astype(f32)
        mixed = tap[0:1] * pads[7 : 7 + tokens] + tap[1:2] * pads[8 : 8 + tokens] + tap[2:3] * pads[9 : 9 + tokens]
        return ((acc_g[:, :128] * inv_rms) * mixed).astype(bf16)

    def expand(d):
        low, high = [], []
        weight = []
        for m in range(chips):
            a, b = latb[d, m, 0].astype(f32), latb[d, m, 1].astype(f32)
            low.append(jnp.where(lane < 64, a, pltpu.roll(b, 64, 1)))
            high.append(jnp.where(lane < 64, pltpu.roll(a, 64, 1), b))
            weight.append(we[pl.ds(pl.multiple_of(chip_of[m] * 128, 128), 128), :])
        weight = jnp.concatenate(weight, axis=0)
        for side, parts in enumerate((low, high)):
            total = sum(p * p for p in parts)
            root = lax.rsqrt(jnp.sum(total, axis=1, keepdims=True) / (128 * chips) + EPSILON)
            parts = [
                (p * root * lat_gain[:, pl.ds(pl.multiple_of(chip_of[m] * 128, 128), 128)]).astype(bf16)
                for m, p in enumerate(parts)
            ]
            result = jnp.dot(jnp.concatenate(parts, axis=1), weight, preferred_element_type=f32).astype(bf16)
            kcat[d, pl.ds(side * half, half), :NOPE] = result[:, :NOPE]
            vals[pl.ds(d * tokens + side * half, half), :] = result[:, NOPE:]

    def score(d):
        if d > 0:
            rope_far[d].wait_recv()
        packed = ropeb[d].astype(f32)
        kcat[d, pl.ds(0, half), NOPE:] = packed.astype(bf16)
        kcat[d, pl.ds(half, half), NOPE:] = pltpu.roll(packed, 64, 1).astype(bf16)
        scores[:, d * tokens : (d + 1) * tokens] = lax.dot_general(
            qcat[...], kcat[d], (((1,), (1,)), ((), ())), preferred_element_type=f32
        )

    conv_mixed = conv()
    previous = None
    for d in order:
        count = pass_lat(d, count)
        if previous is not None:
            for m in range(chips):
                lat_pass[previous, m].wait_recv()
            expand(previous)
            score(previous)
        previous = d
    for m in range(chips):
        lat_pass[previous, m].wait_recv()
    expand(previous)
    score(previous)

    s = scores[...]
    row_max = jnp.max(s, axis=1, keepdims=True)
    e = jnp.exp(s - row_max)
    row_sum = jnp.sum(e, axis=1, keepdims=True)
    summed = jnp.dot(e.astype(bf16), vals[...], preferred_element_type=f32)
    attended = (summed / row_sum).astype(bf16)
    both = jnp.concatenate([attended, conv_mixed], axis=1)

    slice_rows = tokens // (chips * CORES)
    width = wo.shape[1] // OUT_CHUNKS
    pairs, crosses = {}, {}
    for j in range(OUT_CHUNKS):
        cols = pl.ds(j * width, width)
        pbuf[:, cols] = jnp.dot(both, wo[:, cols], preferred_element_type=f32).astype(bf16)
        first, second = (1, 2) if j % 2 == 0 else (2, 1)
        for m in (3, first, second, 0):
            rows = pl.ds(pl.multiple_of((chip_of[m] * CORES + 1 - core) * slice_rows, slice_rows), slice_rows)
            pairs[j, m] = remote(
                pbuf.at[rows, cols], pair_in.at[m, :, cols], pair_send.at[j, m], pair_recv.at[j, m], partner
            )
            pairs[j, m].start()
            pending.append(pairs[j, m])
    lse = row_max + jnp.log(row_sum)
    lse_ref[...] = jnp.transpose(jnp.broadcast_to(lse, (tokens, 128)))[:1]

    def mine(m, cols):
        rows = pl.ds(pl.multiple_of((chip_of[m] * CORES + core) * slice_rows, slice_rows), slice_rows)
        return pbuf[rows, cols].astype(f32) + pair_in[m, :, cols].astype(f32)

    def cross(j, source, target, kind, device):
        copy = remote(source, target, chip_send.at[j, kind], chip_recv.at[j, kind], device)
        copy.start()
        pending.append(copy)
        crosses[j, kind] = copy

    plans = [
        (j, pl.ds(j * width, width)) + ((1, 2) if j % 2 == 0 else (2, 1)) for j in range(OUT_CHUNKS)
    ]
    for j, cols, first, second in plans:
        pairs[j, 3].wait_recv()
        pair_sum[0, :, cols] = mine(3, cols).astype(bf16)
        cross(j, pair_sum.at[0, :, cols], chip_in.at[0, :, cols], 0, mate[first])
        pairs[j, first].wait_recv()
        pair_sum[1, :, cols] = mine(first, cols).astype(bf16)
        cross(j, pair_sum.at[1, :, cols], chip_in.at[1, :, cols], 1, mate[first])
    for j, cols, first, second in plans:
        pairs[j, second].wait_recv()
        crosses[j, 0].wait_recv()
        pair_sum[2, :, cols] = (mine(second, cols) + chip_in[0, :, cols].astype(f32)).astype(bf16)
        cross(j, pair_sum.at[2, :, cols], chip_in.at[2, :, cols], 2, mate[second])
    for j, cols, first, second in plans:
        pairs[j, 0].wait_recv()
        crosses[j, 1].wait_recv()
        total = mine(0, cols) + chip_in[1, :, cols].astype(f32)
        crosses[j, 2].wait_recv()
        out_ref[:, cols] = (total + chip_in[2, :, cols].astype(f32)).astype(bf16)
    for copy in pending:
        copy.wait_send()


def fused(
    mesh,
    activations,
    norm_gain,
    query_weight,
    latent_weight,
    rope_key_weight,
    latent_gain,
    expand_weight,
    gate_weight,
    pre_weight,
    value_weight,
    conv_kernel,
    output_attend,
    output_conv,
):
    splits, chips = mesh.shape["sp"], mesh.shape["tp"] // CORES
    tokens, local = activations.shape
    width = output_attend.shape[1]
    bf16, f32 = jnp.bfloat16, jnp.float32
    slice_rows = tokens // (chips * CORES)
    table = jnp.asarray(rope_table(splits * tokens))
    vmem, hbm = pl.BlockSpec(memory_space=pltpu.VMEM), pl.BlockSpec(memory_space=pltpu.HBM)
    dma = pltpu.SemaphoreType.DMA
    whole = [query_weight.shape[::-1], (latent_weight.shape[1] + rope_key_weight.shape[1], latent_weight.shape[0])]
    whole += [expand_weight.shape, gate_weight.shape, pre_weight.shape, value_weight.shape]
    return pl.pallas_call(
        functools.partial(mixer_kernel, splits, chips),
        out_shape=(
            jax.ShapeDtypeStruct((slice_rows, width), bf16),
            jax.ShapeDtypeStruct((1, tokens), f32),
        ),
        in_specs=[hbm, vmem, hbm, hbm, hbm, vmem, hbm, hbm, hbm, hbm, vmem, hbm, hbm, hbm],
        out_specs=(vmem, vmem),
        scratch_shapes=[pltpu.VMEM((chips, CORES, tokens, local), bf16)]
        + [pltpu.VMEM(shape, bf16) for shape in whole]
        + [
            pltpu.VMEM((output_attend.shape[0] + output_conv.shape[0], width), bf16),
            pltpu.VMEM((tokens, 2 * ROPE), f32),
            pltpu.VMEM((tokens, 128), f32),
            pltpu.VMEM((tokens, 3 * 128), f32),
            pltpu.VMEM((tokens, NOPE + ROPE), f32),
            pltpu.VMEM((splits, chips, CORES, tokens // 2, 128), bf16),
            pltpu.VMEM((splits, tokens // 2, 128), bf16),
            pltpu.VMEM((2, 16, 128), bf16),
            pltpu.VMEM((2, 16, 128), bf16),
            pltpu.VMEM((tokens, 256), bf16),
            pltpu.VMEM((splits, tokens, 256), bf16),
            pltpu.VMEM((splits * tokens, VDIM), bf16),
            pltpu.VMEM((tokens, splits * tokens), f32),
            pltpu.VMEM((tokens + 16, 128), f32),
            pltpu.VMEM((tokens, width), bf16),
            pltpu.VMEM((chips, slice_rows, width), bf16),
            pltpu.VMEM((chips, slice_rows, width), bf16),
            pltpu.VMEM((chips, slice_rows, width), bf16),
            dma((11,)),
            dma((14,)),
            dma((chips, 2, 2)),
            dma((splits * (2 * chips + 1),)),
            dma((splits, chips, 2)),
            dma((splits,)),
            dma((splits,)),
            dma((2,)),
            dma((2,)),
            dma((OUT_CHUNKS, chips)),
            dma((OUT_CHUNKS, chips)),
            dma((OUT_CHUNKS, chips)),
            dma((OUT_CHUNKS, chips)),
        ],
        compiler_params=pltpu.CompilerParams(
            collective_id=0, has_side_effects=True, vmem_limit_bytes=VMEM_LIMIT
        ),
    )(
        activations,
        norm_gain[None],
        query_weight.T,
        latent_weight.T,
        rope_key_weight.T,
        latent_gain[None],
        expand_weight,
        gate_weight,
        pre_weight,
        value_weight,
        conv_kernel,
        output_attend,
        output_conv,
        table,
    )


def solution(mesh):
    return jax.shard_map(
        functools.partial(fused, mesh) if fits(mesh) else body,
        mesh=mesh,
        in_specs=(
            P("sp", "tp"),
            P(),
            P(None, "tp"),
            P(None, "tp"),
            P(),
            P(),
            P(None, "tp"),
            P(None, "tp"),
            P(None, "tp"),
            P(None, "tp"),
            P(None, "tp"),
            P("tp", None),
            P("tp", None),
        ),
        out_specs=(P(("sp", "tp"), None), P("tp", "sp")),
        check_vma=False,
    )
```

```python
import functools
import math

import jax
import jax.numpy as jnp
import numpy as np
from jax import lax
from jax.experimental import pallas as pl
from jax.experimental.pallas import tpu as pltpu
from jax.sharding import PartitionSpec as P

D = 2048
NOPE = 128
ROPE = 64
VDIM = 128
GRID_W = 64


EPSILON = 1e-06
ROPE_BASE = 10000.0


def with_halo(array, sides, width):
    for axis, dim in sides:
        peers, length = (lax.axis_size(axis), array.shape[dim])
        up = [(i, (i + 1) % peers) for i in range(peers - 1)]
        down = [(j, i) for i, j in up]
        last = lax.slice_in_dim(array, length - width, length, axis=dim)
        leading = lax.slice_in_dim(array, 0, width, axis=dim)
        before = lax.ppermute(last, axis, up)
        after = lax.ppermute(leading, axis, down)
        array = jnp.concatenate([before, array, after], axis=dim)
    return array


def rotate(inputs, grid_rows, grid_cols):
    quarter = inputs.shape[-1] // 4
    inverse = ROPE_BASE ** (-jnp.arange(quarter, dtype=jnp.float32) / quarter)
    row_angle = (grid_rows[:, None] * inverse)[:, None, :]
    col_angle = (grid_cols[:, None] * inverse)[:, None, :]
    part_one = inputs[..., :quarter]
    part_two = inputs[..., quarter : 2 * quarter]
    part_three = inputs[..., 2 * quarter : 3 * quarter]
    part_four = inputs[..., 3 * quarter :]
    return jnp.concatenate(
        [
            part_one * jnp.cos(row_angle) - part_two * jnp.sin(row_angle),
            part_one * jnp.sin(row_angle) + part_two * jnp.cos(row_angle),
            part_three * jnp.cos(col_angle) - part_four * jnp.sin(col_angle),
            part_three * jnp.sin(col_angle) + part_four * jnp.cos(col_angle),
        ],
        axis=-1,
    )


def conv_branch(gate_proj, pre_proj, value_proj, conv_kernel):
    pre_mix = (pre_proj * value_proj).astype(jnp.bfloat16)
    padded = with_halo(pre_mix, (("sp", 0),), 1).astype(jnp.float32)
    kernel = conv_kernel.astype(jnp.float32)
    convolved = kernel[0] * padded[:-2] + kernel[1] * padded[1:-1] + kernel[2] * padded[2:]
    return (gate_proj * convolved).astype(jnp.bfloat16)


def body(
    activations,
    norm_gain,
    query_weight,
    latent_weight,
    rope_key_weight,
    latent_gain,
    expand_weight,
    gate_weight,
    pre_weight,
    value_weight,
    conv_kernel,
    output_attend,
    output_conv,
):
    tokens_here = activations.shape[0]
    query_cols = query_weight.shape[1]
    heads_here = query_cols // (NOPE + ROPE)
    latent_cols = latent_weight.shape[1]
    channels = gate_weight.shape[1]
    joined = jnp.concatenate(
        [query_weight, latent_weight, rope_key_weight, gate_weight, pre_weight, value_weight],
        axis=1,
    )
    inputs_f32 = activations.astype(jnp.float32)
    squares = lax.psum(jnp.sum(inputs_f32 * inputs_f32, axis=1, keepdims=True), "tp")
    partial_squares = jnp.zeros((tokens_here, 1), jnp.float32)
    piece_f32 = lax.all_gather(activations, "tp", axis=1, tiled=True).astype(jnp.float32)
    scaled = (piece_f32 * norm_gain).astype(jnp.bfloat16)
    running = jnp.dot(scaled, joined, preferred_element_type=jnp.float32)
    running, folded_squares = (running, partial_squares)
    inv_rms = lax.rsqrt(squares / D + EPSILON)
    projected = running * inv_rms
    latent_end = query_cols + latent_cols
    rope_end = latent_end + ROPE
    query_proj = projected[:, :query_cols]
    latent_proj = projected[:, query_cols:latent_end]
    rope_proj = projected[:, latent_end:rope_end]
    gate_proj = projected[:, rope_end : rope_end + channels]
    pre_proj = projected[:, rope_end + channels : rope_end + 2 * channels]
    value_proj = projected[:, rope_end + 2 * channels :]
    positions = lax.axis_index("sp") * tokens_here + jnp.arange(tokens_here, dtype=jnp.int32)
    grid_rows = (positions // GRID_W).astype(jnp.float32)
    grid_cols = (positions % GRID_W).astype(jnp.float32)
    query = query_proj.reshape(tokens_here, heads_here, NOPE + ROPE)
    query = jnp.concatenate(
        [query[..., :NOPE], rotate(query[..., NOPE:], grid_rows, grid_cols)], axis=-1
    )
    query = (query * (NOPE + ROPE) ** (-0.5)).astype(jnp.bfloat16)
    query_nope = query[..., :NOPE]
    query_rope = query[..., NOPE:]
    gathered = lax.all_gather(latent_proj.astype(jnp.bfloat16), "tp", axis=1, tiled=True).astype(
        jnp.float32
    )
    latent = (
        gathered
        * lax.rsqrt(jnp.mean(gathered * gathered, axis=1, keepdims=True) + EPSILON)
        * latent_gain
    ).astype(jnp.bfloat16)
    expanded = jnp.dot(latent, expand_weight, preferred_element_type=jnp.float32).astype(
        jnp.bfloat16
    )
    rope_key = rotate(rope_proj[:, None, :], grid_rows, grid_cols)[:, 0].astype(jnp.bfloat16)
    starting = (
        jnp.full((heads_here, tokens_here), -jnp.inf, jnp.float32),
        jnp.zeros((heads_here, tokens_here), jnp.float32),
        jnp.zeros((tokens_here, heads_here, VDIM), jnp.float32),
    )
    key_piece = lax.all_gather(expanded, "sp", axis=0, tiled=True)
    rope_piece = lax.all_gather(rope_key, "sp", axis=0, tiled=True)
    piece_rows = key_piece.shape[0]
    key_block = math.gcd(piece_rows, 1024)
    split_heads = key_piece.reshape(piece_rows, heads_here, NOPE + VDIM)

    def one_block(turn_index, state):
        row_max, row_sum, running_out = state
        offset = turn_index * key_block
        block_keys = lax.dynamic_slice_in_dim(split_heads, offset, key_block, 0)
        block_rope = lax.dynamic_slice_in_dim(rope_piece, offset, key_block, 0)
        scores = jnp.einsum(
            "thd,jhd->htj", query_nope, block_keys[..., :NOPE], preferred_element_type=jnp.float32
        )
        scores = scores + jnp.einsum(
            "thd,jd->htj", query_rope, block_rope, preferred_element_type=jnp.float32
        )
        new_max = jnp.maximum(row_max, jnp.max(scores, axis=-1))
        rescale = jnp.exp(row_max - new_max)
        weights = jnp.exp(scores - new_max[..., None])
        row_sum = row_sum * rescale + jnp.sum(weights, axis=-1)
        running_out = running_out * rescale.T[..., None] + jnp.einsum(
            "htj,jhd->thd",
            weights.astype(jnp.bfloat16),
            block_keys[..., NOPE:],
            preferred_element_type=jnp.float32,
        )
        return (new_max, row_sum, running_out)

    row_max, row_sum, running_out = lax.fori_loop(0, piece_rows // key_block, one_block, starting)
    attended = (
        (running_out / row_sum.T[..., None])
        .astype(jnp.bfloat16)
        .reshape(tokens_here, heads_here * VDIM)
    )
    log_weight_sum = row_max + jnp.log(row_sum)
    conv_mixed = conv_branch(gate_proj, pre_proj, value_proj, conv_kernel)
    mixed = lax.psum_scatter(
        (
            jnp.dot(attended, output_attend, preferred_element_type=jnp.float32)
            + jnp.dot(conv_mixed, output_conv, preferred_element_type=jnp.float32)
        ).astype(jnp.bfloat16),
        "tp",
        scatter_dimension=0,
        tiled=True,
    )
    return (mixed, log_weight_sum)


CORES = 2
VMEM_LIMIT = 60 * 2**20
MAX_SPLITS = 8
OUT_CHUNKS = 4
MESH = pl.DeviceIdType.MESH


def fits(mesh):
    chips = mesh.shape["tp"] // CORES
    return mesh.shape["sp"] <= MAX_SPLITS and chips == 4


def flip(index, mask, count):
    total, bit = 0, 1
    while bit < count:
        has = (index // bit) % 2
        total = total + bit * ((1 - has) if mask & bit else has)
        bit *= 2
    return total


def rope_table(tokens):
    quarter = ROPE // 4
    inverse = np.float32(ROPE_BASE) ** (-np.arange(quarter, dtype=np.float32) / np.float32(quarter))
    place = np.arange(tokens)
    row = (place // GRID_W).astype(np.float32)[:, None] * inverse.astype(np.float32)
    col = (place % GRID_W).astype(np.float32)[:, None] * inverse.astype(np.float32)
    parts = [np.cos(row), np.cos(row), np.cos(col), np.cos(col)]
    parts += [-np.sin(row), np.sin(row), -np.sin(col), np.sin(col)]
    return np.concatenate(parts, axis=1).astype(np.float32)


def turn(z, cos, sin):
    lane = lax.broadcasted_iota(jnp.int32, z.shape, 1)
    quarter = ROPE // 4
    other = jnp.where(lane % (2 * quarter) < quarter, pltpu.roll(z, 128 - quarter, 1), pltpu.roll(z, quarter, 1))
    return z * cos + other * sin


def mixer_kernel(
    splits,
    chips,
    act,
    gain,
    wq_h,
    wl_h,
    wr_h,
    lat_gain,
    we_h,
    wg_h,
    wp_h,
    wv_h,
    taps,
    oa_h,
    oc_h,
    tab_h,
    out_ref,
    lse_ref,
    actb,
    wq,
    wlr,
    we,
    wg,
    wp,
    wv,
    wo,
    tab,
    acc_l,
    acc_g,
    acc_q,
    latb,
    ropeb,
    halo_out,
    halo_in,
    qcat,
    kcat,
    vals,
    scores,
    pads,
    pbuf,
    pair_in,
    pair_sum,
    chip_in,
    out_buf,
    in_sem,
    out_sem,
    act_send,
    act_recv,
    lat_send,
    lat_recv,
    rope_send,
    rope_recv,
    halo_send,
    halo_recv,
    pair_send,
    pair_recv,
    chip_send,
    chip_recv,
):
    f32, bf16 = jnp.float32, jnp.bfloat16
    sp, tp = lax.axis_index("sp"), lax.axis_index("tp")
    core, chip = tp % CORES, tp // CORES
    tokens, local = act.shape
    half = tokens // 2
    partner = (sp, chip * CORES + 1 - core)
    chip_of = [flip(chip, m, chips) for m in range(chips)]
    mate = [(sp, chip_of[m] * CORES + core) for m in range(chips)]
    far = [((sp + d) % splits, tp) for d in range(splits)]
    near_first = list(range(1, chips))
    far_first = near_first[::-1]

    def remote(source, target, send, recv, device):
        return pltpu.make_async_remote_copy(
            src_ref=source, dst_ref=target, send_sem=send, recv_sem=recv,
            device_id=device, device_id_type=MESH,
        )

    loads = [
        (act, actb.at[0, core]), (wl_h, wlr.at[pl.ds(0, wl_h.shape[0])]), (wr_h, wlr.at[pl.ds(wl_h.shape[0], wr_h.shape[0])]), (wq_h, wq), (wg_h, wg), (wp_h, wp), (wv_h, wv),
        (tab_h.at[pl.ds(sp * tokens, tokens)], tab), (we_h, we),
        (oa_h, wo.at[pl.ds(0, oa_h.shape[0])]), (oc_h, wo.at[pl.ds(oa_h.shape[0], oc_h.shape[0])]),
    ]
    loads = [pltpu.make_async_copy(a, b, in_sem.at[i]) for i, (a, b) in enumerate(loads)]
    for load in loads:
        load.start()

    barrier = pltpu.get_barrier_semaphore()
    peers = [partner] + mate[1:] + far[1:]
    for peer in peers:
        pl.semaphore_signal(barrier, inc=1, device_id=peer, device_id_type=MESH)
    pl.semaphore_wait(barrier, len(peers))

    pending = []
    loads[0].wait()
    own = actb.at[0, core]

    def act_copy(m, slot, side, kind, device, index):
        piece = pl.ds(side * half, half)
        copy = remote(
            actb.at[m, core, piece], actb.at[slot, core, piece], act_send.at[index], act_recv.at[slot, side, kind], device
        )
        copy.start()
        pending.append(copy)
        return copy

    direct, passed = {}, {}
    for index, (m, side) in enumerate([(1, 0), (2, 1), (1, 1), (2, 0)]):
        direct[m, side] = act_copy(0, m, side, 0, mate[m], index)
    for side in range(2):
        passed[0, side] = act_copy(0, 0, side, 1, partner, 4 + side)
    for load in loads[1:8]:
        load.wait()

    squares = jnp.zeros((tokens, 128), f32)
    scaled = {}

    def rows_of(m, k):
        return pl.ds(pl.multiple_of((chip_of[m] * CORES + k) * local, local), local)

    def scale(m, squares):
        for k in range(CORES):
            x = actb[m, k].astype(f32)
            for c in range(0, local, 128):
                squares = squares + x[:, c : c + 128] * x[:, c : c + 128]
            scaled[m, k] = (x * gain[:, rows_of(m, k)]).astype(bf16)
        return squares

    def put(ref, value, first):
        if first:
            ref[...] = value
        else:
            ref[...] += value

    def across(left, right):
        return lax.dot_general(left, right, (((1,), (1,)), ((), ())), preferred_element_type=f32)

    def latent_dot(m):
        for k in range(CORES):
            rows = rows_of(m, k)
            put(acc_l, across(scaled[m, k], wlr[:, rows]), m == 0 and k == 0)

    def other_dots(m):
        for k in range(CORES):
            rows = rows_of(m, k)
            first = m == 0 and k == 0
            weight = jnp.concatenate([wg[rows, :], wp[rows, :], wv[rows, :]], axis=1)
            put(acc_g, jnp.dot(scaled[m, k], weight, preferred_element_type=f32), first)
            put(acc_q, across(scaled[m, k], wq[:, rows]), first)

    def arrived(m):
        for side in range(2):
            passed[m, side].wait_recv()

    def take(m, squares, others=True):
        arrived(m)
        squares = scale(m, squares)
        latent_dot(m)
        if others:
            other_dots(m)
        return squares

    squares = take(0, squares)
    for index, (m, side) in enumerate([(1, 0), (2, 1), (1, 1), (2, 0)]):
        direct[m, side].wait_recv()
        if index < 2:
            direct[3, side] = act_copy(m, 3, side, 0, mate[3 - m], 6 + index)
        passed[m, side] = act_copy(m, m, side, 1, partner, 8 + index)
    squares = take(1, squares)
    for side in range(2):
        direct[3, side].wait_recv()
        passed[3, side] = act_copy(3, 3, side, 1, partner, 12 + side)
    squares = take(2, squares)
    last = chips - 1
    squares = take(last, squares, False)
    inv_rms = lax.rsqrt(jnp.sum(squares, axis=1, keepdims=True) / (local * chips * CORES) + EPSILON)

    lane = lax.broadcasted_iota(jnp.int32, (half, 128), 1)
    proj = acc_l[...] * inv_rms
    low, high = proj[:half], proj[half:]
    latb[0, 0, core] = jnp.where(lane < 64, low, pltpu.roll(high, 64, 1)).astype(bf16)

    def send_lat(d, m, index, recv, device, slot):
        copy = remote(latb.at[d, m, core], latb.at[slot[0], slot[1], core], lat_send.at[index], recv, device)
        copy.start()
        pending.append(copy)
        return copy

    count = 0
    lat_direct, lat_pass, lat_far = {}, {}, {}
    for d in [d for d in (2, 1, 3) if d < splits] + list(range(4, splits)):
        lat_far[d] = send_lat(0, 0, count, lat_recv.at[(splits - d) % splits, 0, 0], far[d], ((splits - d) % splits, 0))
        count += 1

    def spread(d, count):
        for m in far_first:
            lat_direct[d, m] = send_lat(d, 0, count, lat_recv.at[d, m, 0], mate[m], (d, m))
            count += 1
        lat_pass[d, 0] = send_lat(d, 0, count, lat_recv.at[d, 0, 1], partner, (d, 0))
        return count + 1

    count = spread(0, count)

    table = tab[...]
    wide = lax.broadcasted_iota(jnp.int32, (tokens, 128), 1)
    shifted = pltpu.roll(table, 64, 1)
    cos = jnp.where(wide < 64, table, shifted)
    sin = jnp.where(wide < 64, shifted, table)
    raw = jnp.where(lane < 64, pltpu.roll(low, 64, 1), high)
    ropeb[0] = turn(
        raw,
        jnp.where(lane < 64, cos[:half], cos[half:]),
        jnp.where(lane < 64, sin[:half], sin[half:]),
    ).astype(bf16)
    other_dots(last)

    def far_wait(d):
        lat_far[(splits - d) % splits].wait_recv()

    premix = (acc_g[:, 128:256] * inv_rms) * (acc_g[:, 256:] * inv_rms)
    premix = premix.astype(bf16)
    rim = halo_out.shape[1]
    halo_out[0] = premix[tokens - rim :]
    halo_out[1] = premix[:rim]
    halos = [
        remote(halo_out.at[0], halo_in.at[0], halo_send.at[0], halo_recv.at[0], far[1]),
        remote(halo_out.at[1], halo_in.at[1], halo_send.at[1], halo_recv.at[1], far[splits - 1]),
    ]
    for copy in halos:
        copy.start()
        pending.append(copy)

    rope_far = {}
    for d in range(1, splits):
        back = (splits - d) % splits
        rope_far[back] = remote(ropeb.at[0], ropeb.at[back], rope_send.at[d], rope_recv.at[back], far[d])
        rope_far[back].start()
        pending.append(rope_far[back])

    factor = (NOPE + ROPE) ** (-0.5)
    qcat[:, :NOPE] = (acc_q[:, :NOPE] * inv_rms * factor).astype(bf16)
    tail = jnp.concatenate([acc_q[:, NOPE:], jnp.zeros((tokens, 128 - ROPE), f32)], axis=1) * inv_rms
    qcat[:, NOPE:] = jnp.where(wide < 64, turn(tail, cos, sin) * factor, 0.0).astype(bf16)

    order = [0] + [d for d in (1, 3, 2) if d < splits] + list(range(4, splits))
    for d in order[1:]:
        far_wait(d)
        count = spread(d, count)

    for load in loads[8:]:
        load.wait()

    def pass_lat(d, count):
        for m in near_first:
            lat_direct[d, m].wait_recv()
            lat_pass[d, m] = send_lat(d, m, count, lat_recv.at[d, m, 1], partner, (d, m))
            count += 1
        return count

    def conv():
        pads[8 : 8 + tokens] = premix.astype(f32)
        for copy in halos:
            copy.wait_recv()
        before = jnp.where(sp > 0, halo_in[0].astype(f32)[rim - 1 :], 0.0)
        after = jnp.where(sp < splits - 1, halo_in[1].astype(f32)[:1], 0.0)
        pads[7:8] = before
        pads[8 + tokens : 9 + tokens] = after
        tap = taps[...].astype(f32)
        mixed = tap[0:1] * pads[7 : 7 + tokens] + tap[1:2] * pads[8 : 8 + tokens] + tap[2:3] * pads[9 : 9 + tokens]
        return ((acc_g[:, :128] * inv_rms) * mixed).astype(bf16)

    def expand(d):
        low, high = [], []
        weight = []
        for m in range(chips):
            a, b = latb[d, m, 0].astype(f32), latb[d, m, 1].astype(f32)
            low.append(jnp.where(lane < 64, a, pltpu.roll(b, 64, 1)))
            high.append(jnp.where(lane < 64, pltpu.roll(a, 64, 1), b))
            weight.append(we[pl.ds(pl.multiple_of(chip_of[m] * 128, 128), 128), :])
        weight = jnp.concatenate(weight, axis=0)
        for side, parts in enumerate((low, high)):
            total = sum(p * p for p in parts)
            root = lax.rsqrt(jnp.sum(total, axis=1, keepdims=True) / (128 * chips) + EPSILON)
            parts = [
                (p * root * lat_gain[:, pl.ds(pl.multiple_of(chip_of[m] * 128, 128), 128)]).astype(bf16)
                for m, p in enumerate(parts)
            ]
            result = jnp.dot(jnp.concatenate(parts, axis=1), weight, preferred_element_type=f32).astype(bf16)
            kcat[d, pl.ds(side * half, half), :NOPE] = result[:, :NOPE]
            vals[pl.ds(d * tokens + side * half, half), :] = result[:, NOPE:]

    def score(d):
        if d > 0:
            rope_far[d].wait_recv()
        packed = ropeb[d].astype(f32)
        kcat[d, pl.ds(0, half), NOPE:] = packed.astype(bf16)
        kcat[d, pl.ds(half, half), NOPE:] = pltpu.roll(packed, 64, 1).astype(bf16)
        scores[:, d * tokens : (d + 1) * tokens] = lax.dot_general(
            qcat[...], kcat[d], (((1,), (1,)), ((), ())), preferred_element_type=f32
        )

    previous = None
    for d in order:
        count = pass_lat(d, count)
        if previous is not None:
            for m in range(chips):
                lat_pass[previous, m].wait_recv()
            expand(previous)
            score(previous)
        previous = d
    conv_mixed = conv()
    for m in range(chips):
        lat_pass[previous, m].wait_recv()
    expand(previous)
    score(previous)

    s = scores[...]
    row_max = jnp.max(s, axis=1, keepdims=True)
    e = jnp.exp(s - row_max)
    row_sum = jnp.sum(e, axis=1, keepdims=True)
    summed = jnp.dot(e.astype(bf16), vals[...], preferred_element_type=f32)
    attended = (summed / row_sum).astype(bf16)
    both = jnp.concatenate([attended, conv_mixed], axis=1)

    slice_rows = tokens // (chips * CORES)
    width = wo.shape[1] // OUT_CHUNKS
    pairs, crosses = {}, {}
    for j in range(OUT_CHUNKS):
        cols = pl.ds(j * width, width)
        pbuf[:, cols] = jnp.dot(both, wo[:, cols], preferred_element_type=f32).astype(bf16)
        first, second = (1, 2) if j % 2 == 0 else (2, 1)
        for m in (3, first, second, 0):
            rows = pl.ds(pl.multiple_of((chip_of[m] * CORES + 1 - core) * slice_rows, slice_rows), slice_rows)
            pairs[j, m] = remote(
                pbuf.at[rows, cols], pair_in.at[m, :, cols], pair_send.at[j, m], pair_recv.at[j, m], partner
            )
            pairs[j, m].start()
            pending.append(pairs[j, m])
    lse = row_max + jnp.log(row_sum)
    lse_ref[...] = jnp.transpose(jnp.broadcast_to(lse, (tokens, 128)))[:1]

    def mine(m, cols):
        rows = pl.ds(pl.multiple_of((chip_of[m] * CORES + core) * slice_rows, slice_rows), slice_rows)
        return pbuf[rows, cols].astype(f32) + pair_in[m, :, cols].astype(f32)

    def cross(j, source, target, kind, device):
        copy = remote(source, target, chip_send.at[j, kind], chip_recv.at[j, kind], device)
        copy.start()
        pending.append(copy)
        crosses[j, kind] = copy

    stores = []
    plans = [
        (j, pl.ds(j * width, width)) + ((1, 2) if j % 2 == 0 else (2, 1)) for j in range(OUT_CHUNKS)
    ]
    for j, cols, first, second in plans:
        pairs[j, 3].wait_recv()
        pair_sum[0, :, cols] = mine(3, cols).astype(bf16)
        cross(j, pair_sum.at[0, :, cols], chip_in.at[0, :, cols], 0, mate[first])
        pairs[j, first].wait_recv()
        pair_sum[1, :, cols] = mine(first, cols).astype(bf16)
        cross(j, pair_sum.at[1, :, cols], chip_in.at[1, :, cols], 1, mate[first])
    for j, cols, first, second in plans:
        pairs[j, second].wait_recv()
        crosses[j, 0].wait_recv()
        pair_sum[2, :, cols] = (mine(second, cols) + chip_in[0, :, cols].astype(f32)).astype(bf16)
        cross(j, pair_sum.at[2, :, cols], chip_in.at[2, :, cols], 2, mate[second])
    for j, cols, first, second in plans:
        pairs[j, 0].wait_recv()
        crosses[j, 1].wait_recv()
        total = mine(0, cols) + chip_in[1, :, cols].astype(f32)
        crosses[j, 2].wait_recv()
        out_buf[:, cols] = (total + chip_in[2, :, cols].astype(f32)).astype(bf16)
        copy = pltpu.make_async_copy(out_buf.at[:, cols], out_ref.at[:, cols], out_sem.at[j])
        copy.start()
        stores.append(copy)
    for copy in pending:
        copy.wait_send()
    for copy in stores:
        copy.wait()


def fused(
    mesh,
    activations,
    norm_gain,
    query_weight,
    latent_weight,
    rope_key_weight,
    latent_gain,
    expand_weight,
    gate_weight,
    pre_weight,
    value_weight,
    conv_kernel,
    output_attend,
    output_conv,
):
    splits, chips = mesh.shape["sp"], mesh.shape["tp"] // CORES
    tokens, local = activations.shape
    width = output_attend.shape[1]
    bf16, f32 = jnp.bfloat16, jnp.float32
    slice_rows = tokens // (chips * CORES)
    table = jnp.asarray(rope_table(splits * tokens))
    vmem, hbm = pl.BlockSpec(memory_space=pltpu.VMEM), pl.BlockSpec(memory_space=pltpu.HBM)
    dma = pltpu.SemaphoreType.DMA
    whole = [query_weight.shape[::-1], (latent_weight.shape[1] + rope_key_weight.shape[1], latent_weight.shape[0])]
    whole += [expand_weight.shape, gate_weight.shape, pre_weight.shape, value_weight.shape]
    return pl.pallas_call(
        functools.partial(mixer_kernel, splits, chips),
        out_shape=(
            jax.ShapeDtypeStruct((slice_rows, width), bf16),
            jax.ShapeDtypeStruct((1, tokens), f32),
        ),
        in_specs=[hbm, vmem, hbm, hbm, hbm, vmem, hbm, hbm, hbm, hbm, vmem, hbm, hbm, hbm],
        out_specs=(hbm, vmem),
        scratch_shapes=[pltpu.VMEM((chips, CORES, tokens, local), bf16)]
        + [pltpu.VMEM(shape, bf16) for shape in whole]
        + [
            pltpu.VMEM((output_attend.shape[0] + output_conv.shape[0], width), bf16),
            pltpu.VMEM((tokens, 2 * ROPE), f32),
            pltpu.VMEM((tokens, 128), f32),
            pltpu.VMEM((tokens, 3 * 128), f32),
            pltpu.VMEM((tokens, NOPE + ROPE), f32),
            pltpu.VMEM((splits, chips, CORES, tokens // 2, 128), bf16),
            pltpu.VMEM((splits, tokens // 2, 128), bf16),
            pltpu.VMEM((2, 16, 128), bf16),
            pltpu.VMEM((2, 16, 128), bf16),
            pltpu.VMEM((tokens, 256), bf16),
            pltpu.VMEM((splits, tokens, 256), bf16),
            pltpu.VMEM((splits * tokens, VDIM), bf16),
            pltpu.VMEM((tokens, splits * tokens), f32),
            pltpu.VMEM((tokens + 16, 128), f32),
            pltpu.VMEM((tokens, width), bf16),
            pltpu.VMEM((chips, slice_rows, width), bf16),
            pltpu.VMEM((chips, slice_rows, width), bf16),
            pltpu.VMEM((chips, slice_rows, width), bf16),
            pltpu.VMEM((slice_rows, width), bf16),
            dma((11,)),
            dma((OUT_CHUNKS,)),
            dma((14,)),
            dma((chips, 2, 2)),
            dma((splits * (2 * chips + 1),)),
            dma((splits, chips, 2)),
            dma((splits,)),
            dma((splits,)),
            dma((2,)),
            dma((2,)),
            dma((OUT_CHUNKS, chips)),
            dma((OUT_CHUNKS, chips)),
            dma((OUT_CHUNKS, chips)),
            dma((OUT_CHUNKS, chips)),
        ],
        compiler_params=pltpu.CompilerParams(
            collective_id=0, has_side_effects=True, vmem_limit_bytes=VMEM_LIMIT
        ),
    )(
        activations,
        norm_gain[None],
        query_weight.T,
        latent_weight.T,
        rope_key_weight.T,
        latent_gain[None],
        expand_weight,
        gate_weight,
        pre_weight,
        value_weight,
        conv_kernel,
        output_attend,
        output_conv,
        table,
    )


def solution(mesh):
    return jax.shard_map(
        functools.partial(fused, mesh) if fits(mesh) else body,
        mesh=mesh,
        in_specs=(
            P("sp", "tp"),
            P(),
            P(None, "tp"),
            P(None, "tp"),
            P(),
            P(),
            P(None, "tp"),
            P(None, "tp"),
            P(None, "tp"),
            P(None, "tp"),
            P(None, "tp"),
            P("tp", None),
            P("tp", None),
        ),
        out_specs=(P(("sp", "tp"), None), P("tp", "sp")),
        check_vma=False,
    )
```
